32 devices in a mesh: sp: 8 (over z, y), tp: 4 (over x, core).
Axes of the slice: x: 2, y: 2, z: 4, core: 2. Of those that a mesh axis runs over, the one named last changes fastest.
Arguments:
- out_grad: bfloat16 [2048, 4096], P('sp'), may hold values from -6 to 6
- stream: bfloat16 [2048, 4096], P('sp'), may hold values from -6 to 6
- norm_gain: bfloat16 [4096], replicated, may hold values from 0.099609375 to 1.8984375
- routes: int32 [2048, 2], P('sp'), may hold values from 0 to 7, all different within a row; in each aligned block of 256 rows (0 to 255, 256 to 511, ...) at most 80 rows name the same one
- route_weight: float32 [2048, 2], P('sp'), may hold values from 0.3 to 1.5
- gate_weight: bfloat16 [8, 4096, 1024], P('sp', None, 'tp'), may hold values from -0.09375 to 0.09375
- up_weight: bfloat16 [8, 4096, 1024], P('sp', None, 'tp'), may hold values from -0.09375 to 0.09375
- down_weight: bfloat16 [8, 1024, 4096], P('sp', 'tp'), may hold values from -0.1875 to 0.1875
- out_proj: bfloat16 [4096, 1024], P(None, 'tp'), may hold values from -0.1875 to 0.1875
- conv_out: bfloat16 [2048, 1024], P('sp', 'tp'), as said below
- gate_branch: bfloat16 [2048, 1024], P('sp', 'tp'), may hold values from -6 to 6
- decay_map: bfloat16 [2, 4, 256, 256], P(None, 'tp'), as said below
- input_map: bfloat16 [2, 4, 256, 256], P(None, 'tp'), as said below
- decay_param: float32 [2, 1024], P(None, 'tp'), as said below
- decay_shift: float32 [2, 2048, 1024], P(None, 'sp', 'tp'), as said below
- states: float32 [2, 2048, 1024], P(None, 'sp', 'tp'), as said below
Outputs:
- conv_grad: float32 [2048, 1024], P('sp', 'tp')
- gate_branch_grad: float32 [2048, 1024], P('sp', 'tp')
- out_proj_grad: float32 [4096, 1024], P('sp', 'tp')
- gate_weight_grad: bfloat16 [8, 4096, 1024], P('sp', None, 'tp')
- up_weight_grad: bfloat16 [8, 4096, 1024], P('sp', None, 'tp')
- down_weight_grad: bfloat16 [8, 1024, 4096], P('sp', 'tp')
The draws below stay inside these ranges and needn't reach their ends.
Inputs may be any that keep to these rules, and one draw needn't show every extreme that they name: `routes`: each token names 2 different experts. Among the 256 tokens of one index of sp no expert is named more than 80 times, a bound that some expert reaches in some of these blocks. `conv_out`: within -6 to 6. `decay_map`: entries within -4 to 4 times 256 to the power -0.5. `input_map`: entries within -4 to 4 times 256 to the power -0.5. `decay_param`: between 3.7 and 3.5 plus the logarithm of 2048. `decay_shift`: every entry lies between -0.7 and -0.00002. The forward pass's states: they follow the recurrences of the steps from conv_out, decay_map, input_map, decay_param and decay_shift.
All inputs are finite; a program needn't handle non-finite values.
Results may differ from the reference program's by a relative error of at most 0.018.
Values may be sent and summed in bfloat16 or wider, within the bound.
A program may use at most 128 MiB of HBM per device.

```python
import math
import jax
import jax.numpy as jnp
import numpy as np
from jax import lax

D = 4096
RECURRENT_WIDTH = 1024
BLOCKS = 4
BW = 256
FF = 1024
TOP = 2
TOK_DEV = 256
EXPERTS = 8
SEQUENCE_TOKENS = 2048
CAP = 80
N_SP = 8
N_TP = 4


def scan_pairs(coeffs, values, reverse):

    def combine(earlier, later):
        return (earlier[0] * later[0], later[0] * earlier[1] + later[1])
    return lax.associative_scan(combine, (coeffs, values), axis=0, reverse=reverse)[1]


def block_apply(channels, block_maps):
    shaped = channels.reshape(channels.shape[0], block_maps.shape[0], block_maps.shape[1])
    mapped = jnp.einsum('tkc,kcd->tkd', shaped, block_maps.astype(jnp.float32), precision=lax.Precision.HIGHEST)
    return mapped.reshape(channels.shape)


def lru_draw(key):
    random_keys = jax.random.split(jax.random.fold_in(key, 4242), 9)
    conv_field = jax.random.normal(random_keys[1], (SEQUENCE_TOKENS, RECURRENT_WIDTH), jnp.float32)
    fast_share = 0.5
    conv_field = jnp.clip(conv_field, -6.0, 6.0).astype(jnp.bfloat16)
    gate_maps = jnp.clip(jax.random.normal(random_keys[2], (2, 2, BLOCKS, BW, BW), jnp.float32), -4.0, 4.0)
    gate_maps = (gate_maps * BW ** (-0.5)).astype(jnp.bfloat16)
    fast_mask = jax.random.uniform(random_keys[3], (2, RECURRENT_WIDTH), jnp.float32) < fast_share
    slow_values = jnp.log(SEQUENCE_TOKENS * 1.0) + jax.random.uniform(random_keys[4], (2, RECURRENT_WIDTH), jnp.float32, 2.0, 3.5)
    fast_values = jax.random.uniform(random_keys[5], (2, RECURRENT_WIDTH), jnp.float32, 3.7, 4.9)
    decay_values = jnp.where(fast_mask, fast_values, slow_values)
    block_count = SEQUENCE_TOKENS // TOK_DEV
    block_rate = jnp.exp(jax.random.uniform(random_keys[6], (2, block_count), jnp.float32, -10.6, -9.2))
    shift_offset = -jnp.repeat(block_rate, TOK_DEV, axis=1)[:, :, None]
    spike_mask = jax.random.uniform(random_keys[7], (2, SEQUENCE_TOKENS, RECURRENT_WIDTH), jnp.float32) < 1.5 / SEQUENCE_TOKENS
    spike_depth = jnp.log(jax.random.uniform(random_keys[8], (2, SEQUENCE_TOKENS, RECURRENT_WIDTH), jnp.float32, 0.5, 0.8))
    offset_field = shift_offset + jnp.where(spike_mask, spike_depth, 0.0)
    conv_float = conv_field.astype(jnp.float32)
    state_list = []
    for direction in range(2):
        decay_gate = jax.nn.sigmoid(block_apply(conv_float, gate_maps[0, direction]))
        input_gate = jax.nn.sigmoid(block_apply(conv_float, gate_maps[1, direction]))
        log_decay = -8.0 * decay_gate * jax.nn.softplus(-decay_values[direction])[None, :] + offset_field[direction]
        drive_term = jnp.sqrt(-jnp.expm1(2.0 * log_decay)) * input_gate * conv_float
        state_list.append(scan_pairs(jnp.exp(log_decay), drive_term, direction == 1))
    return (conv_field, gate_maps[0], gate_maps[1], decay_values, offset_field, jnp.stack(state_list))


def draw_conv_out(key, part):
    return lru_draw(key)[0]


def draw_decay_map(key, part):
    return lru_draw(key)[1]


def draw_input_map(key, part):
    return lru_draw(key)[2]


def draw_decay_param(key, part):
    return lru_draw(key)[3]


def draw_decay_shift(key, part):
    return lru_draw(key)[4]


def draw_states(key, part):
    return lru_draw(key)[5]


def raised(values, rng, source, target, blocks, factor):
    owner, partner = [(jnp.arange(values.shape[position]) // (values.shape[position] // blocks)).reshape([-1 if axis == position else 1 for axis in range(values.ndim)]) for position in (source, target)]
    chosen = jax.random.permutation(rng, blocks)[partner]
    strong = (owner == chosen) | (owner == (partner + blocks // 2) % blocks)
    return jnp.where(strong, factor * values, values)


def levels(key, dims, pieces, least, largest):
    loudness = 1.0
    for position, parts in pieces:
        heights = jax.random.uniform(jax.random.fold_in(jax.random.fold_in(key, 6), position), (parts,), jnp.float32, least / len(pieces), largest / len(pieces))
        loudness = loudness * jnp.repeat(jnp.exp(heights), dims[position] // parts).reshape((-1,) + (1,) * (len(dims) - 1 - position))
    return loudness


def deal_out(key, own, number, rows, number_of, top, most, lean):
    order = jax.random.permutation(key, number_of)
    crowded, common = load_shares(number_of, rows * top, most, lean, True), load_shares(number_of, rows * top, most, lean, False)
    places = jnp.arange(number_of)

    def named(tallies, offset_by):
        used = int((tallies > 0).sum())
        fixed = max(1, used // 4)
        shifted = fixed + (places - fixed + offset_by * (used - fixed)) % max(1, number_of - fixed)
        return jnp.zeros((number_of,), jnp.int32).at[order[jnp.where(places < fixed, places, shifted)]].set(jnp.asarray(tallies, jnp.int32))

    tallies = jnp.where(number % 4 == 0, named(crowded, number // 4), named(common, number - number // 4 - 1))
    mixed = jax.random.permutation(jax.random.fold_in(own, 3), number_of)
    donor, sink = mixed[0:number_of // 2 * 2:2], mixed[1:number_of // 2 * 2:2]
    room = jnp.minimum(tallies[donor] - 1, most - tallies[sink]) // 2
    room = jnp.where((donor == order[0]) | (sink == order[0]) | (tallies[sink] == 0), 0, jnp.maximum(room, 0))
    shifted = jax.random.randint(jax.random.fold_in(own, 4), (number_of // 2,), 0, 1 << 20) % (room + 1)
    tallies = tallies.at[donor].add(-shifted).at[sink].add(shifted)
    members = jnp.searchsorted(jnp.cumsum(tallies), jnp.arange(rows * top), side="right").astype(jnp.int32)
    grid = members.reshape(top, rows).T
    grid = grid[jax.random.permutation(jax.random.fold_in(own, 1), rows)]
    offset_by = jax.random.randint(jax.random.fold_in(own, 2), (rows, 1), 0, top)
    return jnp.take_along_axis(grid, (jnp.arange(top)[None, :] + offset_by) % top, axis=1)


def load_shares(count, total, limit, skew, full):
    loads = [(1 << 20) // math.isqrt(standing ** skew) + 1 for standing in range(1, count + 1)]
    largest = limit if full else min(limit, max(-(-total // count), total * loads[0] // sum(loads)))
    least = 1 if total - largest >= count - 1 else 0
    counts, rest = [largest] + [least] * (count - 1), total - largest - least * (count - 1)
    while rest > 0:
        movable = [i for i in range(1, count) if counts[i] < largest] or [i for i in range(1, count) if counts[i] < limit]
        whole, remaining = sum([loads[i] for i in movable]), rest
        for i in movable:
            more = min(limit - counts[i], max(1, remaining * loads[i] // whole), rest)
            counts[i] = counts[i] + more
            rest = rest - more
    return np.array(counts)


def bell_draw(stream_key, shape, deviation, reach, shards=(), held_as=jnp.bfloat16):
    drawn = deviation * jax.random.normal(stream_key, shape, jnp.float32)
    if shards:
        drawn = drawn * levels(stream_key, shape, shards, -0.22, 0.18)
    return jnp.clip(drawn, -reach, reach).astype(held_as)


def noise_with(own_key, dims, deviation, most, cuts, heavy, kind=jnp.bfloat16):
    array = deviation * jax.random.normal(own_key, dims, jnp.float32)
    if cuts:
        array = array * levels(own_key, dims, cuts, -0.22, 0.18)
    return jnp.clip(raised(array, jax.random.fold_in(own_key, 3), *heavy), -most, most).astype(kind)


def setup_inputs(seed: int = 0) -> dict:
    key_of = jax.random.split(jax.random.key(seed), 17)
    out_grad = noise_with(key_of[0], (SEQUENCE_TOKENS, D), 1.0, 6.0, ((0, 8),), (0, 1, 8, 2.0))
    stream = bell_draw(key_of[1], (SEQUENCE_TOKENS, D), 1.0, 6.0, ((0, 8),))
    norm_gain = jnp.clip(1.0 + 0.18 * jax.random.normal(key_of[2], (D,), jnp.float32), 0.099609375, 1.8984375).astype(jnp.bfloat16)
    routes_keys = jax.random.split(jax.random.fold_in(key_of[3], 1), SEQUENCE_TOKENS // TOK_DEV)
    routes_turns = jax.random.permutation(jax.random.fold_in(key_of[3], 3), SEQUENCE_TOKENS // TOK_DEV)
    routes = jax.vmap(lambda own, number: deal_out(jax.random.fold_in(key_of[3], 2), own, number, TOK_DEV, EXPERTS, TOP, CAP, 1))(routes_keys, routes_turns).reshape((SEQUENCE_TOKENS, TOP))
    route_weight = jnp.clip(0.3 + 1.2 * jax.random.uniform(key_of[4], (SEQUENCE_TOKENS, TOP), jnp.float32) ** levels(key_of[4], (SEQUENCE_TOKENS, TOP), ((0, 8),), -0.2, 0.2), 0.3, 1.5)
    gate_weight = bell_draw(key_of[5], (EXPERTS, D, FF), D ** -0.5, 0.09375, ((0, 8), (2, 4)))
    up_weight = bell_draw(key_of[6], (EXPERTS, D, FF), D ** -0.5, 0.09375, ((0, 8), (2, 4)))
    down_weight = bell_draw(key_of[7], (EXPERTS, FF, D), FF ** -0.5, 0.1875, ((0, 8), (1, 4)))
    out_proj = bell_draw(key_of[8], (D, RECURRENT_WIDTH), RECURRENT_WIDTH ** -0.5, 0.1875, ((1, 4),))
    conv_out = draw_conv_out(jax.random.fold_in(key_of[16], 71), 0)
    gate_branch = bell_draw(key_of[10], (SEQUENCE_TOKENS, RECURRENT_WIDTH), 1.0, 6.0, ((0, 8), (1, 4)))
    decay_map = draw_decay_map(jax.random.fold_in(key_of[16], 71), 0)
    input_map = draw_input_map(jax.random.fold_in(key_of[16], 71), 0)
    decay_param = draw_decay_param(jax.random.fold_in(key_of[16], 71), 0)
    decay_shift = draw_decay_shift(jax.random.fold_in(key_of[16], 71), 0)
    states = draw_states(jax.random.fold_in(key_of[16], 71), 0)
    return dict(out_grad=out_grad, stream=stream, norm_gain=norm_gain, routes=routes, route_weight=route_weight, gate_weight=gate_weight, up_weight=up_weight, down_weight=down_weight, out_proj=out_proj, conv_out=conv_out, gate_branch=gate_branch, decay_map=decay_map, input_map=input_map, decay_param=decay_param, decay_shift=decay_shift, states=states)


rate_scale = 8.0
norm_eps = 1e-06

def contract(left, right, left_dim, right_dim):
    return lax.dot_general(left, right, (((left_dim,), (right_dim,)), ((), ())), preferred_element_type=jnp.float32)

def linear_scan(coeffs, values, reverse):

    def combine(earlier, later):
        return (earlier[0] * later[0], later[0] * earlier[1] + later[1])
    return lax.associative_scan(combine, (coeffs, values), axis=0, reverse=reverse)

def silu_grad(values):
    logistic = jax.nn.sigmoid(values)
    return logistic * (1.0 + values * (1.0 - logistic))

def expert_pass(slot_inputs, slot_cotan, gate_local, up_local, down_local):
    gate_pre = contract(slot_inputs, gate_local, 1, 0)
    up_pre = contract(slot_inputs, up_local, 1, 0)
    hidden = (jax.nn.silu(gate_pre) * up_pre).astype(jnp.bfloat16)
    down_wgrad = contract(hidden, slot_cotan, 0, 0)
    hidden_grad = contract(slot_cotan, down_local, 1, 1)
    up_grad = (hidden_grad * jax.nn.silu(gate_pre)).astype(jnp.bfloat16)
    gate_grad = (hidden_grad * up_pre * silu_grad(gate_pre)).astype(jnp.bfloat16)
    gate_wgrad = contract(slot_inputs, gate_grad, 0, 0)
    up_wgrad = contract(slot_inputs, up_grad, 0, 0)
    return (gate_wgrad, up_wgrad, down_wgrad, gate_grad, up_grad)

def block_forward(channels, block_maps):
    shaped = channels.reshape(channels.shape[0], block_maps.shape[0], block_maps.shape[1])
    mapped = jnp.einsum('tkc,kcd->tkd', shaped, block_maps.astype(jnp.float32), precision=lax.Precision.HIGHEST)
    return mapped.reshape(channels.shape)

def block_backward(pre_grad, block_maps):
    shaped = pre_grad.reshape(pre_grad.shape[0], block_maps.shape[0], block_maps.shape[2])
    mapped = jnp.einsum('tkd,kcd->tkc', shaped, block_maps.astype(jnp.float32), precision=lax.Precision.HIGHEST)
    return mapped.reshape(pre_grad.shape)

def recurrence_back(adjoint, state_run, conv_float, gate_parts, decay_local, input_local):
    decay_gate, input_gate, decay_base, decay_rate, drive_scale, drive_term = gate_parts
    log_grad = adjoint * (state_run - drive_term) - adjoint * input_gate * conv_float * decay_rate * decay_rate / drive_scale
    decay_pre_grad = log_grad * (-rate_scale * decay_base) * decay_gate * (1.0 - decay_gate)
    input_pre_grad = adjoint * drive_scale * conv_float * input_gate * (1.0 - input_gate)
    return adjoint * drive_scale * input_gate + block_backward(decay_pre_grad, decay_local) + block_backward(input_pre_grad, input_local)

def reference(out_grad, stream, norm_gain, routes, route_weight, gate_weight, up_weight, down_weight, out_proj, conv_out, gate_branch, decay_map, input_map, decay_param, decay_shift, states):
    stream_f = stream.astype(jnp.float32)
    row_scale = lax.rsqrt(lax.optimization_barrier(jnp.mean(stream_f * stream_f, axis=1, keepdims=True)) + norm_eps)
    unit_rows = stream_f * row_scale
    gain_row = norm_gain.astype(jnp.float32)[None, :]
    normed = (unit_rows * gain_row).astype(jnp.bfloat16)
    pair_count = SEQUENCE_TOKENS * TOP
    pair_expert = routes.reshape(N_SP, TOK_DEV * TOP)
    onehot = (pair_expert[:, :, None] == jnp.arange(EXPERTS, dtype=jnp.int32)[None, None, :]).astype(jnp.int32)
    slot_rank = lax.optimization_barrier(jnp.sum((jnp.cumsum(onehot, axis=1) - onehot) * onehot, axis=2))
    source = jnp.arange(N_SP, dtype=jnp.int32)[:, None]
    slot_index = (pair_expert * (N_SP * CAP) + source * CAP + slot_rank).reshape(-1).astype(jnp.int32)
    slot_pair = jnp.full((EXPERTS * N_SP * CAP,), pair_count, jnp.int32).at[slot_index].set(jnp.arange(pair_count, dtype=jnp.int32))
    slot_token = (slot_pair // TOP).astype(jnp.int32)
    zero_row = jnp.zeros((1, D), jnp.bfloat16)
    slot_inputs = jnp.concatenate([normed, zero_row])[slot_token].reshape(EXPERTS, N_SP * CAP, D)
    weight_pad = jnp.concatenate([route_weight.reshape(-1), jnp.zeros((1,), jnp.float32)])
    slot_cotan = (weight_pad[slot_pair][:, None] * jnp.concatenate([out_grad, zero_row])[slot_token].astype(jnp.float32)).astype(jnp.bfloat16)
    slot_cotan = slot_cotan.reshape(EXPERTS, N_SP * CAP, D)

    def one_expert(operands):
        inputs_e, cotan_e, gate_local, up_local, down_local = operands
        gate_wgrad, up_wgrad, down_wgrad, gate_grad, up_grad = expert_pass(inputs_e, cotan_e, gate_local, up_local, down_local)
        run_width = FF // N_TP
        total_sum = jnp.zeros((inputs_e.shape[0], D), jnp.float32)
        for quarter in range(N_TP):
            low_unit = quarter * run_width
            high_unit = low_unit + run_width
            partial_value = contract(gate_grad[:, low_unit:high_unit], gate_local[:, low_unit:high_unit], 1, 1) + contract(up_grad[:, low_unit:high_unit], up_local[:, low_unit:high_unit], 1, 1)
            total_sum = total_sum + lax.optimization_barrier(partial_value.astype(jnp.bfloat16)).astype(jnp.float32)
        return (gate_wgrad.astype(jnp.bfloat16), up_wgrad.astype(jnp.bfloat16), down_wgrad.astype(jnp.bfloat16), total_sum.astype(jnp.bfloat16))
    gate_grads, up_grads, down_grads, pair_grad = lax.map(one_expert, (slot_inputs, slot_cotan, gate_weight, up_weight, down_weight))
    returned = pair_grad.reshape(EXPERTS * N_SP * CAP, D)[slot_index]
    normed_grad = lax.optimization_barrier(jnp.sum(returned.reshape(SEQUENCE_TOKENS, TOP, D).astype(jnp.float32), axis=1))
    scaled_grad = gain_row * normed_grad
    stream_grad = out_grad.astype(jnp.float32) + row_scale * (scaled_grad - unit_rows * lax.optimization_barrier(jnp.mean(unit_rows * scaled_grad, axis=1, keepdims=True)))
    stream_grad_b = stream_grad.astype(jnp.bfloat16)
    total_state = states[0] + states[1]
    gate_float = gate_branch.astype(jnp.float32)
    gelu_gate, gelu_back = jax.vjp(jax.nn.gelu, gate_float)
    lru_out = (total_state * gelu_gate).astype(jnp.bfloat16)
    out_proj_grad = contract(stream_grad_b, lru_out, 0, 0)
    lru_out_grad = contract(stream_grad_b, out_proj, 1, 0)
    gate_branch_grad = gelu_back(lru_out_grad * total_state)[0]
    state_grad = lru_out_grad * gelu_gate
    conv_float = conv_out.astype(jnp.float32)
    ones_row = jnp.ones((1, RECURRENT_WIDTH), jnp.float32)
    conv_grad = jnp.zeros_like(conv_float)
    for direction in range(2):
        decay_gate = jax.nn.sigmoid(block_forward(conv_float, decay_map[direction]))
        input_gate = jax.nn.sigmoid(block_forward(conv_float, input_map[direction]))
        decay_base = jax.nn.softplus(-decay_param[direction])[None, :]
        log_decay = -rate_scale * decay_gate * decay_base + decay_shift[direction]
        decay_rate = jnp.exp(log_decay)
        drive_scale = jnp.sqrt(-jnp.expm1(2.0 * log_decay))
        drive_term = drive_scale * input_gate * conv_float
        if direction == 0:
            adjoint = linear_scan(jnp.concatenate([decay_rate[1:], ones_row]), state_grad, True)[1]
        else:
            adjoint = linear_scan(jnp.concatenate([ones_row, decay_rate[:-1]]), state_grad, False)[1]
        gate_parts = (decay_gate, input_gate, decay_base, decay_rate, drive_scale, drive_term)
        conv_grad = conv_grad + recurrence_back(adjoint, states[direction], conv_float, gate_parts, decay_map[direction], input_map[direction])
    return (conv_grad, gate_branch_grad, out_proj_grad, gate_grads, up_grads, down_grads)
```

```python
import jax
import jax.numpy as jnp
from jax import lax
from jax.sharding import PartitionSpec as P

TOP = 2
EXP_DEV = 1
TOK_DEV = 256


rate_scale = 8.0
norm_eps = 1e-06


def contract(left, right, left_dim, right_dim):
    return lax.dot_general(
        left, right, (((left_dim,), (right_dim,)), ((), ())), preferred_element_type=jnp.float32
    )


def linear_scan(coeffs, values, reverse):

    def combine(earlier, later):
        return (earlier[0] * later[0], later[0] * earlier[1] + later[1])

    return lax.associative_scan(combine, (coeffs, values), axis=0, reverse=reverse)


def silu_grad(values):
    logistic = jax.nn.sigmoid(values)
    return logistic * (1.0 + values * (1.0 - logistic))


def expert_pass(slot_inputs, slot_cotan, gate_local, up_local, down_local):
    gate_pre = contract(slot_inputs, gate_local, 1, 0)
    up_pre = contract(slot_inputs, up_local, 1, 0)
    hidden = (jax.nn.silu(gate_pre) * up_pre).astype(jnp.bfloat16)
    down_wgrad = contract(hidden, slot_cotan, 0, 0)
    hidden_grad = contract(slot_cotan, down_local, 1, 1)
    up_grad = (hidden_grad * jax.nn.silu(gate_pre)).astype(jnp.bfloat16)
    gate_grad = (hidden_grad * up_pre * silu_grad(gate_pre)).astype(jnp.bfloat16)
    gate_wgrad = contract(slot_inputs, gate_grad, 0, 0)
    up_wgrad = contract(slot_inputs, up_grad, 0, 0)
    return (gate_wgrad, up_wgrad, down_wgrad, gate_grad, up_grad)


def block_forward(channels, block_maps):
    shaped = channels.reshape(channels.shape[0], block_maps.shape[0], block_maps.shape[1])
    mapped = jnp.einsum("tkc,kcd->tkd", shaped, block_maps, preferred_element_type=jnp.float32)
    return mapped.reshape(channels.shape)


def block_backward(pre_grad, block_maps):
    shaped = pre_grad.reshape(pre_grad.shape[0], block_maps.shape[0], block_maps.shape[2])
    mapped = jnp.einsum(
        "tkd,kcd->tkc", shaped, block_maps.astype(jnp.float32), precision=lax.Precision.HIGHEST
    )
    return mapped.reshape(pre_grad.shape)


def recurrence_back(adjoint, state_run, conv_float, gate_parts, decay_local, input_local):
    decay_gate, input_gate, decay_base, decay_rate, drive_scale, drive_term = gate_parts
    log_grad = (
        adjoint * (state_run - drive_term)
        - adjoint * input_gate * conv_float * decay_rate * decay_rate / drive_scale
    )
    decay_pre_grad = log_grad * (-rate_scale * decay_base) * decay_gate * (1.0 - decay_gate)
    input_pre_grad = adjoint * drive_scale * conv_float * input_gate * (1.0 - input_gate)
    return (
        adjoint * drive_scale * input_gate
        + block_backward(decay_pre_grad, decay_local)
        + block_backward(input_pre_grad, input_local)
    )


def body(
    out_grad,
    stream,
    norm_gain,
    routes,
    route_weight,
    gate_weight,
    up_weight,
    down_weight,
    out_proj,
    conv_out,
    gate_branch,
    decay_map,
    input_map,
    decay_param,
    decay_shift,
    states,
):
    sources = lax.axis_size("sp")
    quarters = lax.axis_size("tp")
    experts = EXP_DEV * sources
    capacity = (5 * TOP * TOK_DEV + 4 * experts - 1) // (4 * experts)
    token_count, model_width = stream.shape
    stream_f = stream.astype(jnp.float32)
    row_scale = lax.rsqrt(jnp.mean(stream_f * stream_f, axis=1, keepdims=True) + norm_eps)
    unit_rows = stream_f * row_scale
    gain_row = norm_gain.astype(jnp.float32)[None, :]
    normed = (unit_rows * gain_row).astype(jnp.bfloat16)
    pair_expert = routes.reshape(-1)
    pair_count = pair_expert.shape[0]
    onehot = (pair_expert[:, None] == jnp.arange(experts, dtype=jnp.int32)[None, :]).astype(
        jnp.int32
    )
    slot_rank = jnp.sum((jnp.cumsum(onehot, axis=0) - onehot) * onehot, axis=1)
    slot_index = pair_expert * capacity + slot_rank
    slot_pair = (
        jnp.full((experts * capacity,), pair_count, jnp.int32)
        .at[slot_index]
        .set(jnp.arange(pair_count, dtype=jnp.int32))
    )
    slot_token = slot_pair // TOP
    weight_pad = jnp.concatenate([route_weight.reshape(-1), jnp.zeros((1,), jnp.float32)])
    slot_weight = weight_pad[slot_pair][:, None]
    column_width = model_width // quarters
    column_start = lax.axis_index("tp") * column_width
    normed_cols = lax.dynamic_slice_in_dim(normed, column_start, column_width, 1)
    zero_row = jnp.zeros((1, normed_cols.shape[1]), jnp.bfloat16)
    slot_inputs = jnp.concatenate([normed_cols, zero_row])[slot_token]
    slot_cotan = (
        slot_weight
        * jnp.concatenate(
            [lax.dynamic_slice_in_dim(out_grad, column_start, column_width, 1), zero_row]
        )[slot_token].astype(jnp.float32)
    ).astype(jnp.bfloat16)
    part_inputs, part_cotan = (
        lax.all_to_all(slot_inputs, "sp", split_axis=0, concat_axis=0, tiled=True),
        lax.all_to_all(slot_cotan, "sp", split_axis=0, concat_axis=0, tiled=True),
    )
    got_inputs, got_cotan = (
        lax.all_gather(part_inputs, "tp", axis=1, tiled=True),
        lax.all_gather(part_cotan, "tp", axis=1, tiled=True),
    )

    def by_expert(slot_block):
        shaped = slot_block.reshape(sources, EXP_DEV, capacity, model_width)
        return jnp.swapaxes(shaped, 0, 1).reshape(EXP_DEV, sources * capacity, model_width)

    expert_inputs = by_expert(got_inputs)
    expert_cotan = by_expert(got_cotan)
    gate_grads, up_grads, down_grads, partials = ([], [], [], [])
    gate_wgrad, up_wgrad, down_wgrad, gate_grad, up_grad = expert_pass(
        expert_inputs[0], expert_cotan[0], gate_weight[0], up_weight[0], down_weight[0]
    )
    gate_grads.append(gate_wgrad.astype(jnp.bfloat16))
    up_grads.append(up_wgrad.astype(jnp.bfloat16))
    down_grads.append(down_wgrad.astype(jnp.bfloat16))
    partials.append(
        (contract(gate_grad, gate_weight[0], 1, 1) + contract(up_grad, up_weight[0], 1, 1)).astype(
            jnp.bfloat16
        )
    )
    partial_slots = jnp.swapaxes(
        jnp.stack(partials).reshape(EXP_DEV, sources, capacity, model_width), 0, 1
    )
    partial_slots = partial_slots.reshape(sources * EXP_DEV * capacity, model_width)
    summed = (
        lax.psum_scatter(partial_slots, "tp", scatter_dimension=1, tiled=True)
        .astype(jnp.float32)
        .astype(jnp.bfloat16)
    )
    part_back = lax.all_to_all(summed, "sp", split_axis=0, concat_axis=0, tiled=True)
    quarter_grad = jnp.sum(
        part_back[slot_index].reshape(token_count, TOP, column_width).astype(jnp.float32), axis=1
    ).astype(jnp.bfloat16)
    normed_grad = lax.all_gather(quarter_grad, "tp", axis=1, tiled=True).astype(jnp.float32)
    scaled_grad = gain_row * normed_grad
    stream_grad = out_grad.astype(jnp.float32) + row_scale * (
        scaled_grad - unit_rows * jnp.mean(unit_rows * scaled_grad, axis=1, keepdims=True)
    )
    stream_grad_b = stream_grad.astype(jnp.bfloat16)
    total_state = states[0] + states[1]
    gate_float = gate_branch.astype(jnp.float32)
    gelu_gate, gelu_back = jax.vjp(jax.nn.gelu, gate_float)
    lru_out = (total_state * gelu_gate).astype(jnp.bfloat16)
    lru_rows = lax.all_gather(lru_out, "sp", axis=0, tiled=True)
    piece_width = column_width // sources
    own_piece = lax.dynamic_slice_in_dim(
        stream_grad_b.reshape(token_count, sources, quarters, piece_width),
        lax.axis_index("tp"),
        1,
        2,
    )[:, :, 0]
    piece_rows = lax.all_to_all(jnp.swapaxes(own_piece, 0, 1), "sp", split_axis=0, concat_axis=0, tiled=True)
    grad_rows = lax.all_gather(
        piece_rows.reshape(sources * token_count, piece_width), "tp", axis=1, tiled=True
    )
    out_proj_grad = contract(grad_rows, lru_rows, 0, 0)
    lru_out_grad = contract(stream_grad_b, out_proj, 1, 0)
    gate_branch_grad = gelu_back(lru_out_grad * total_state)[0]
    state_grad = lru_out_grad * gelu_gate
    conv_float = conv_out.astype(jnp.float32)
    ones_row = jnp.ones((1, conv_float.shape[1]), jnp.float32)
    saved, summaries = ([], [])
    for direction in range(2):
        decay_gate = jax.nn.sigmoid(block_forward(conv_out, decay_map[direction]))
        input_gate = jax.nn.sigmoid(block_forward(conv_out, input_map[direction]))
        decay_base = jax.nn.softplus(-decay_param[direction])[None, :]
        log_decay = -rate_scale * decay_gate * decay_base + decay_shift[direction]
        decay_rate = jnp.exp(log_decay)
        drive_scale = jnp.sqrt(-jnp.expm1(2.0 * log_decay))
        drive_term = drive_scale * input_gate * conv_float
        if direction == 0:
            reach_coeff, inner_sum = linear_scan(
                jnp.concatenate([decay_rate[1:], ones_row]), state_grad, True
            )
            summaries.append(decay_rate[:1] * reach_coeff[:1])
            summaries.append(decay_rate[:1] * inner_sum[:1])
        else:
            reach_coeff, inner_sum = linear_scan(
                jnp.concatenate([ones_row, decay_rate[:-1]]), state_grad, False
            )
            summaries.append(decay_rate[-1:] * reach_coeff[-1:])
            summaries.append(decay_rate[-1:] * inner_sum[-1:])
        saved.append(
            (
                (decay_gate, input_gate, decay_base, decay_rate, drive_scale, drive_term),
                reach_coeff,
                inner_sum,
            )
        )
    gathered = lax.all_gather(jnp.concatenate(summaries, axis=0), "sp", axis=1, tiled=False)
    device_index = lax.axis_index("sp")
    zero_row = jnp.zeros_like(ones_row)
    from_right = linear_scan(gathered[0], gathered[1], True)[1]
    from_left = linear_scan(gathered[2], gathered[3], False)[1]
    incoming = (
        lax.dynamic_slice_in_dim(jnp.concatenate([from_right[1:], zero_row]), device_index, 1, 0),
        lax.dynamic_slice_in_dim(jnp.concatenate([zero_row, from_left[:-1]]), device_index, 1, 0),
    )
    conv_grad = jnp.zeros_like(conv_float)
    for direction in range(2):
        gate_parts, reach_coeff, inner_sum = saved[direction]
        adjoint = inner_sum + reach_coeff * incoming[direction]
        conv_grad = conv_grad + recurrence_back(
            adjoint,
            states[direction],
            conv_float,
            gate_parts,
            decay_map[direction],
            input_map[direction],
        )
    return (
        conv_grad,
        gate_branch_grad,
        out_proj_grad,
        jnp.stack(gate_grads),
        jnp.stack(up_grads),
        jnp.stack(down_grads),
    )


def solution(mesh):
    placed = (
        P("sp", None),
        P("sp", None),
        P(),
        P("sp", None),
        P("sp", None),
        P("sp", None, "tp"),
        P("sp", None, "tp"),
        P("sp", "tp", None),
        P(None, "tp"),
        P("sp", "tp"),
        P("sp", "tp"),
        P(None, "tp", None, None),
        P(None, "tp", None, None),
        P(None, "tp"),
        P(None, "sp", "tp"),
        P(None, "sp", "tp"),
    )
    return jax.shard_map(
        body,
        mesh=mesh,
        in_specs=placed,
        out_specs=(
            P("sp", "tp"),
            P("sp", "tp"),
            P("sp", "tp"),
            P("sp", None, "tp"),
            P("sp", None, "tp"),
            P("sp", "tp", None),
        ),
        check_vma=False,
    )
```

```python
import functools

import jax
import jax.numpy as jnp
from jax import lax
from jax.experimental import pallas as pl
from jax.experimental.pallas import tpu as pltpu
from jax.sharding import PartitionSpec as P

TOP = 2
EXP_DEV = 1
TOK_DEV = 256


rate_scale = 8.0
norm_eps = 1e-06


def contract(left, right, left_dim, right_dim):
    return lax.dot_general(
        left, right, (((left_dim,), (right_dim,)), ((), ())), preferred_element_type=jnp.float32
    )


def linear_scan(coeffs, values, reverse):

    def combine(earlier, later):
        return (earlier[0] * later[0], later[0] * earlier[1] + later[1])

    return lax.associative_scan(combine, (coeffs, values), axis=0, reverse=reverse)


def silu_grad(values):
    logistic = jax.nn.sigmoid(values)
    return logistic * (1.0 + values * (1.0 - logistic))


def expert_pass(slot_inputs, slot_cotan, gate_local, up_local, down_local):
    gate_pre = contract(slot_inputs, gate_local, 1, 0)
    up_pre = contract(slot_inputs, up_local, 1, 0)
    hidden = (jax.nn.silu(gate_pre) * up_pre).astype(jnp.bfloat16)
    down_wgrad = contract(hidden, slot_cotan, 0, 0)
    hidden_grad = contract(slot_cotan, down_local, 1, 1)
    up_grad = (hidden_grad * jax.nn.silu(gate_pre)).astype(jnp.bfloat16)
    gate_grad = (hidden_grad * up_pre * silu_grad(gate_pre)).astype(jnp.bfloat16)
    gate_wgrad = contract(slot_inputs, gate_grad, 0, 0)
    up_wgrad = contract(slot_inputs, up_grad, 0, 0)
    return (gate_wgrad, up_wgrad, down_wgrad, gate_grad, up_grad)


def block_forward(channels, block_maps):
    shaped = channels.reshape(channels.shape[0], block_maps.shape[0], block_maps.shape[1])
    mapped = jnp.einsum("tkc,kcd->tkd", shaped, block_maps, preferred_element_type=jnp.float32)
    return mapped.reshape(channels.shape)


def block_backward(pre_grad, block_maps):
    shaped = pre_grad.reshape(pre_grad.shape[0], block_maps.shape[0], block_maps.shape[2])
    mapped = jnp.einsum(
        "tkd,kcd->tkc", shaped, block_maps.astype(jnp.float32), precision=lax.Precision.HIGHEST
    )
    return mapped.reshape(pre_grad.shape)


def recurrence_back(adjoint, state_run, conv_float, gate_parts, decay_local, input_local):
    decay_gate, input_gate, decay_base, decay_rate, drive_scale, drive_term = gate_parts
    log_grad = (
        adjoint * (state_run - drive_term)
        - adjoint * input_gate * conv_float * decay_rate * decay_rate / drive_scale
    )
    decay_pre_grad = log_grad * (-rate_scale * decay_base) * decay_gate * (1.0 - decay_gate)
    input_pre_grad = adjoint * drive_scale * conv_float * input_gate * (1.0 - input_gate)
    return (
        adjoint * drive_scale * input_gate
        + block_backward(decay_pre_grad, decay_local)
        + block_backward(input_pre_grad, input_local)
    )


MESH = pl.DeviceIdType.MESH


def push(source, target, send_sem, recv_sem, where):
    return pltpu.make_async_remote_copy(
        src_ref=source,
        dst_ref=target,
        send_sem=send_sem,
        recv_sem=recv_sem,
        device_id=where,
        device_id_type=MESH,
    )


def greet(sources, me, others):
    barrier = pltpu.get_barrier_semaphore()

    def one(step, carry):
        pl.semaphore_signal(
            barrier, inc=1, device_id={"sp": lax.rem(me + step, sources)}, device_id_type=MESH
        )
        return carry

    lax.fori_loop(1, sources, one, 0)
    for other in others:
        pl.semaphore_signal(barrier, inc=1, device_id={"tp": other}, device_id_type=MESH)
    pl.semaphore_wait(barrier, sources - 1 + len(others))


def loop(low, high, step):
    def one(index, carry):
        step(index)
        return carry

    lax.fori_loop(low, high, one, 0)


def quarter_at(ref, slot, quarter, width):
    return ref.at[slot, :, pl.ds(pl.multiple_of(quarter * width, width), width)]


def dispatch_kernel(
    sources, in_ref, ct_ref, oin_ref, oct_ref,
    send_a, recv_a, send_b, recv_b, send_c, recv_c, send_d, recv_d, local
):
    me, mine = lax.axis_index("sp"), lax.axis_index("tp")
    beside = mine + 1 - 2 * lax.rem(mine, 2)
    across = lax.rem(mine + 2, 4)
    diagonal = lax.rem(beside + 2, 4)
    width = in_ref.shape[2]
    pairs = ((in_ref, oin_ref), (ct_ref, oct_ref))
    owned = [
        pltpu.make_async_copy(src.at[me], quarter_at(dst, me, mine, width), local.at[arr])
        for arr, (src, dst) in enumerate(pairs)
    ]
    for copy in owned:
        copy.start()
    greet(sources, me, (beside, across))

    def first(arr, peer):
        src, dst = pairs[arr]
        return push(
            src.at[peer], quarter_at(dst, me, mine, width),
            send_a.at[arr, peer], recv_a.at[arr, me], {"sp": peer},
        )

    def first_landed(arr, origin):
        src, dst = pairs[arr]
        return push(
            src.at[me], quarter_at(dst, origin, mine, width),
            send_a.at[arr, me], recv_a.at[arr, origin], {"sp": origin},
        )

    def passed(arr, slot, quarter, send, recv, target):
        view = quarter_at(pairs[arr][1], slot, quarter, width)
        return push(view, view, send.at[arr, slot], recv.at[arr, slot], {"tp": target})

    def start_first(step):
        peer = lax.rem(me + step, sources)
        first(0, peer).start()
        first(1, peer).start()

    loop(1, sources, start_first)
    for copy in owned:
        copy.wait()

    def relay(slot):
        for arr in range(2):
            passed(arr, slot, mine, send_c, recv_c, across).start()
            passed(arr, slot, mine, send_b, recv_b, beside).start()

    relay(me)

    def onward(step):
        slot = lax.rem(me + sources - step, sources)
        for arr in range(2):
            passed(arr, slot, across, send_c, recv_c, across).wait_recv()
            passed(arr, slot, across, send_d, recv_d, beside).start()

    lag = 2

    def steps(step):
        @pl.when(step < sources)
        def _():
            slot = lax.rem(me + sources - step, sources)
            for arr in range(2):
                first_landed(arr, slot).wait_recv()
            relay(slot)

        @pl.when(step >= lag)
        def _():
            onward(step - lag)

    loop(1, sources + lag, steps)

    def finish(slot):
        for arr in range(2):
            passed(arr, slot, beside, send_b, recv_b, beside).wait_recv()
            passed(arr, slot, diagonal, send_d, recv_d, beside).wait_recv()
            passed(arr, slot, mine, send_b, recv_b, beside).wait_send()
            passed(arr, slot, mine, send_c, recv_c, across).wait_send()
            passed(arr, slot, across, send_d, recv_d, beside).wait_send()

    loop(0, sources, finish)

    def finish_first(step):
        peer = lax.rem(me + step, sources)
        for arr in range(2):
            first(arr, peer).wait_send()

    loop(1, sources, finish_first)


def dispatch(sources, slot_inputs, slot_cotan):
    _, capacity, width = slot_inputs.shape
    rows = jax.ShapeDtypeStruct((sources, capacity, 4 * width), slot_inputs.dtype)
    two = pltpu.SemaphoreType.DMA((2, sources))
    return pl.pallas_call(
        functools.partial(dispatch_kernel, sources),
        out_shape=(rows, rows),
        in_specs=[pl.BlockSpec(memory_space=pltpu.VMEM)] * 2,
        out_specs=[pl.BlockSpec(memory_space=pl.ANY)] * 2,
        scratch_shapes=[two] * 8 + [pltpu.SemaphoreType.DMA((2,))],
        compiler_params=pltpu.CompilerParams(collective_id=0, has_side_effects=True),
    )(slot_inputs, slot_cotan)


def return_kernel(
    sources, part_ref, lru_ref, out_ref, olru_ref, near, paired, distant, total,
    send_a, recv_a, send_b, recv_b, send_c, recv_c, send_l, recv_l, local
):
    me, mine = lax.axis_index("sp"), lax.axis_index("tp")
    beside = mine + 1 - 2 * lax.rem(mine, 2)
    across = lax.rem(mine + 2, 4)
    diagonal = lax.rem(beside + 2, 4)
    width = total.shape[2]
    greet(sources, me, (beside, across))

    def load(slot, quarter):
        columns = pl.ds(pl.multiple_of(quarter * width, width), width)
        return part_ref[slot, :, columns].astype(jnp.float32)

    def near_copy(slot, place, quarter):
        return push(
            quarter_at(part_ref, slot, quarter, width), near.at[slot, place],
            send_a.at[slot, place], recv_a.at[slot, place], {"tp": beside},
        )

    def far_copy(slot):
        return push(
            paired.at[slot], distant.at[slot], send_b.at[slot], recv_b.at[slot], {"tp": across}
        )

    def home_copy(peer, slot):
        return push(
            total.at[peer], out_ref.at[slot], send_c.at[peer], recv_c.at[slot], {"sp": peer}
        )

    def own_copy():
        return pltpu.make_async_copy(total.at[me], out_ref.at[me], local.at[0])

    def lru_copy(peer, slot):
        return push(lru_ref, olru_ref.at[slot], send_l.at[peer], recv_l.at[slot], {"sp": peer})

    def start_lru(step):
        peer = lax.rem(me + step, sources)
        lru_copy(peer, me).start()

    lru_own = pltpu.make_async_copy(lru_ref, olru_ref.at[me], local.at[1])
    lru_own.start()
    def begin(step):
        slot = lax.rem(me + 1 + step, sources)
        near_copy(slot, 1, diagonal).start()
        near_copy(slot, 0, beside).start()

    loop(0, sources, begin)
    loop(1, sources, start_lru)
    lag = 2

    def steps(step):
        @pl.when(step < sources)
        def _():
            slot = lax.rem(me + 1 + step, sources)
            near_copy(slot, 1, diagonal).wait_recv()
            paired[slot] = (load(slot, across) + near[slot, 1].astype(jnp.float32)).astype(
                jnp.bfloat16
            )
            far_copy(slot).start()

        @pl.when(step >= lag)
        def _():
            slot = lax.rem(me + 1 + step - lag, sources)
            near_copy(slot, 0, beside).wait_recv()
            far_copy(slot).wait_recv()
            total[slot] = (
                load(slot, mine)
                + near[slot, 0].astype(jnp.float32)
                + distant[slot].astype(jnp.float32)
            ).astype(jnp.bfloat16)

            @pl.when(step < sources + lag - 1)
            def _():
                home_copy(slot, me).start()

    loop(0, sources + lag, steps)
    own_copy().start()

    def finish(step):
        peer = lax.rem(me + step, sources)
        home_copy(peer, peer).wait_recv()
        home_copy(peer, me).wait_send()
        lru_copy(peer, me).wait_send()
        lru_copy(peer, peer).wait_recv()

    loop(1, sources, finish)

    def finish_tp(slot):
        near_copy(slot, 0, beside).wait_send()
        near_copy(slot, 1, diagonal).wait_send()
        far_copy(slot).wait_send()

    loop(0, sources, finish_tp)
    own_copy().wait()
    lru_own.wait()


def return_rows(sources, partial, lru_out):
    _, capacity, model_width = partial.shape
    width = model_width // 4
    held = pltpu.VMEM((sources, capacity, width), jnp.bfloat16)
    two = pltpu.SemaphoreType.DMA((sources, 2))
    one = pltpu.SemaphoreType.DMA((sources,))
    return pl.pallas_call(
        functools.partial(return_kernel, sources),
        out_shape=(
            jax.ShapeDtypeStruct((sources, capacity, width), jnp.bfloat16),
            jax.ShapeDtypeStruct((sources,) + lru_out.shape, lru_out.dtype),
        ),
        in_specs=[pl.BlockSpec(memory_space=pltpu.VMEM)] * 2,
        out_specs=[pl.BlockSpec(memory_space=pl.ANY)] * 2,
        scratch_shapes=[
            pltpu.VMEM((sources, 2, capacity, width), jnp.bfloat16), held, held, held,
            two, two, one, one, one, one, one, one, pltpu.SemaphoreType.DMA((2,)),
        ],
        compiler_params=pltpu.CompilerParams(collective_id=1, has_side_effects=True),
    )(partial, lru_out)


def share_kernel(sources, own_ref, out_ref, send_a, recv_a):
    me = lax.axis_index("sp")
    greet(sources, me, ())
    out_ref[me] = own_ref[...]

    def copy(peer, slot):
        return push(own_ref, out_ref.at[slot], send_a.at[peer], recv_a.at[slot], {"sp": peer})

    loop(1, sources, lambda step: copy(lax.rem(me + step, sources), me).start())

    def finish(step):
        peer = lax.rem(me + step, sources)
        copy(peer, peer).wait_recv()
        copy(peer, me).wait_send()

    loop(1, sources, finish)


def share(sources, own):
    one = pltpu.SemaphoreType.DMA((sources,))
    return pl.pallas_call(
        functools.partial(share_kernel, sources),
        out_shape=jax.ShapeDtypeStruct((sources,) + own.shape, own.dtype),
        in_specs=[pl.BlockSpec(memory_space=pltpu.VMEM)],
        out_specs=pl.BlockSpec(memory_space=pltpu.VMEM),
        scratch_shapes=[one, one],
        compiler_params=pltpu.CompilerParams(collective_id=2, has_side_effects=True),
    )(own)


def body(
    out_grad,
    stream,
    norm_gain,
    routes,
    route_weight,
    gate_weight,
    up_weight,
    down_weight,
    out_proj,
    conv_out,
    gate_branch,
    decay_map,
    input_map,
    decay_param,
    decay_shift,
    states,
):
    sources = lax.axis_size("sp")
    quarters = lax.axis_size("tp")
    experts = EXP_DEV * sources
    capacity = (5 * TOP * TOK_DEV + 4 * experts - 1) // (4 * experts)
    token_count, model_width = stream.shape
    stream_f = stream.astype(jnp.float32)
    row_scale = lax.rsqrt(jnp.mean(stream_f * stream_f, axis=1, keepdims=True) + norm_eps)
    unit_rows = stream_f * row_scale
    gain_row = norm_gain.astype(jnp.float32)[None, :]
    normed = (unit_rows * gain_row).astype(jnp.bfloat16)
    pair_expert = routes.reshape(-1)
    pair_count = pair_expert.shape[0]
    onehot = (pair_expert[:, None] == jnp.arange(experts, dtype=jnp.int32)[None, :]).astype(
        jnp.int32
    )
    slot_rank = jnp.sum((jnp.cumsum(onehot, axis=0) - onehot) * onehot, axis=1)
    slot_index = pair_expert * capacity + slot_rank
    places = slot_index.reshape(token_count, TOP, 1) == jnp.arange(
        experts * capacity, dtype=jnp.int32
    )
    chosen = jnp.any(places, axis=1).astype(jnp.bfloat16)
    slot_weight = jnp.sum(jnp.where(places, route_weight[:, :, None], 0.0), axis=(0, 1))[:, None]
    column_width = model_width // quarters
    column_start = lax.axis_index("tp") * column_width
    normed_cols = lax.dynamic_slice_in_dim(normed, column_start, column_width, 1)
    grad_cols = lax.dynamic_slice_in_dim(out_grad, column_start, column_width, 1)
    slot_inputs = contract(chosen, normed_cols, 0, 0).astype(jnp.bfloat16)
    slot_cotan = (slot_weight * contract(chosen, grad_cols, 0, 0)).astype(jnp.bfloat16)
    total_state = states[0] + states[1]
    gate_float = gate_branch.astype(jnp.float32)
    gelu_gate, gelu_back = jax.vjp(jax.nn.gelu, gate_float)
    lru_out = (total_state * gelu_gate).astype(jnp.bfloat16)
    got_inputs, got_cotan = dispatch(
        sources,
        slot_inputs.reshape(sources, capacity, column_width),
        slot_cotan.reshape(sources, capacity, column_width),
    )
    expert_inputs = got_inputs.reshape(1, sources * capacity, model_width)
    expert_cotan = got_cotan.reshape(1, sources * capacity, model_width)
    gate_grads, up_grads, down_grads, partials = ([], [], [], [])
    gate_wgrad, up_wgrad, down_wgrad, gate_grad, up_grad = expert_pass(
        expert_inputs[0], expert_cotan[0], gate_weight[0], up_weight[0], down_weight[0]
    )
    gate_grads.append(gate_wgrad.astype(jnp.bfloat16))
    up_grads.append(up_wgrad.astype(jnp.bfloat16))
    down_grads.append(down_wgrad.astype(jnp.bfloat16))
    partials.append(
        (contract(gate_grad, gate_weight[0], 1, 1) + contract(up_grad, up_weight[0], 1, 1)).astype(
            jnp.bfloat16
        )
    )
    part_back, lru_rows = return_rows(
        sources, partials[0].reshape(sources, capacity, model_width), lru_out
    )
    lru_rows = lru_rows.reshape(sources * token_count, lru_out.shape[1])
    quarter_grad = contract(
        chosen, part_back.reshape(sources * capacity, column_width), 1, 0
    ).astype(jnp.bfloat16)
    normed_grad = lax.all_gather(quarter_grad, "tp", axis=1, tiled=True).astype(jnp.float32)
    scaled_grad = gain_row * normed_grad
    stream_grad = out_grad.astype(jnp.float32) + row_scale * (
        scaled_grad - unit_rows * jnp.mean(unit_rows * scaled_grad, axis=1, keepdims=True)
    )
    stream_grad_b = stream_grad.astype(jnp.bfloat16)
    piece_width = column_width // sources
    own_piece = lax.dynamic_slice_in_dim(
        stream_grad_b.reshape(token_count, sources, quarters, piece_width),
        lax.axis_index("tp"),
        1,
        2,
    )[:, :, 0]
    piece_rows = lax.all_to_all(jnp.swapaxes(own_piece, 0, 1), "sp", split_axis=0, concat_axis=0, tiled=True)
    grad_rows = lax.all_gather(
        piece_rows.reshape(sources * token_count, piece_width), "tp", axis=1, tiled=True
    )
    out_proj_grad = contract(grad_rows, lru_rows, 0, 0)
    lru_out_grad = contract(stream_grad_b, out_proj, 1, 0)
    gate_branch_grad = gelu_back(lru_out_grad * total_state)[0]
    state_grad = lru_out_grad * gelu_gate
    conv_float = conv_out.astype(jnp.float32)
    ones_row = jnp.ones((1, conv_float.shape[1]), jnp.float32)
    saved, summaries = ([], [])
    for direction in range(2):
        decay_gate = jax.nn.sigmoid(block_forward(conv_out, decay_map[direction]))
        input_gate = jax.nn.sigmoid(block_forward(conv_out, input_map[direction]))
        decay_base = jax.nn.softplus(-decay_param[direction])[None, :]
        log_decay = -rate_scale * decay_gate * decay_base + decay_shift[direction]
        decay_rate = jnp.exp(log_decay)
        drive_scale = jnp.sqrt(-jnp.expm1(2.0 * log_decay))
        drive_term = drive_scale * input_gate * conv_float
        if direction == 0:
            reach_coeff, inner_sum = linear_scan(
                jnp.concatenate([decay_rate[1:], ones_row]), state_grad, True
            )
            summaries.append(decay_rate[:1] * reach_coeff[:1])
            summaries.append(decay_rate[:1] * inner_sum[:1])
        else:
            reach_coeff, inner_sum = linear_scan(
                jnp.concatenate([ones_row, decay_rate[:-1]]), state_grad, False
            )
            summaries.append(decay_rate[-1:] * reach_coeff[-1:])
            summaries.append(decay_rate[-1:] * inner_sum[-1:])
        saved.append(
            (
                (decay_gate, input_gate, decay_base, decay_rate, drive_scale, drive_term),
                reach_coeff,
                inner_sum,
            )
        )
    gathered = jnp.swapaxes(share(sources, jnp.concatenate(summaries, axis=0)), 0, 1)
    device_index = lax.axis_index("sp")
    zero_row = jnp.zeros_like(ones_row)
    from_right = linear_scan(gathered[0], gathered[1], True)[1]
    from_left = linear_scan(gathered[2], gathered[3], False)[1]
    incoming = (
        lax.dynamic_slice_in_dim(jnp.concatenate([from_right[1:], zero_row]), device_index, 1, 0),
        lax.dynamic_slice_in_dim(jnp.concatenate([zero_row, from_left[:-1]]), device_index, 1, 0),
    )
    conv_grad = jnp.zeros_like(conv_float)
    for direction in range(2):
        gate_parts, reach_coeff, inner_sum = saved[direction]
        adjoint = inner_sum + reach_coeff * incoming[direction]
        conv_grad = conv_grad + recurrence_back(
            adjoint,
            states[direction],
            conv_float,
            gate_parts,
            decay_map[direction],
            input_map[direction],
        )
    return (
        conv_grad,
        gate_branch_grad,
        out_proj_grad,
        jnp.stack(gate_grads),
        jnp.stack(up_grads),
        jnp.stack(down_grads),
    )


def solution(mesh):
    placed = (
        P("sp", None),
        P("sp", None),
        P(),
        P("sp", None),
        P("sp", None),
        P("sp", None, "tp"),
        P("sp", None, "tp"),
        P("sp", "tp", None),
        P(None, "tp"),
        P("sp", "tp"),
        P("sp", "tp"),
        P(None, "tp", None, None),
        P(None, "tp", None, None),
        P(None, "tp"),
        P(None, "sp", "tp"),
        P(None, "sp", "tp"),
    )
    return jax.shard_map(
        body,
        mesh=mesh,
        in_specs=placed,
        out_specs=(
            P("sp", "tp"),
            P("sp", "tp"),
            P("sp", "tp"),
            P("sp", None, "tp"),
            P("sp", None, "tp"),
            P("sp", "tp", None),
        ),
        check_vma=False,
    )
```
